32 devices in a mesh: fs: 8 (over z, x), tp: 4 (over y, core).
Axes of the slice: x: 2, y: 2, z: 4, core: 2. Of those that a mesh axis runs over, the one named last changes fastest.
Arguments:
- tokens: bfloat16 [8192, 2048], P('fs', 'tp'), may hold values from -17 to 17
- first_gain: float32 [2048], replicated, may hold values from 0.1 to 1.9
- first_gate: bfloat16 [2048, 5120], P('fs', 'tp'), may hold values from -0.125 to 0.125
- first_up: bfloat16 [2048, 5120], P('fs', 'tp'), may hold values from -0.125 to 0.125
- first_down: bfloat16 [2048, 5120], P('fs', 'tp'), may hold values from -0.078125 to 0.078125
- mix_gain: float32 [2048], replicated, may hold values from 0.1 to 1.9
- mix_input: bfloat16 [2048, 1024], P('fs', 'tp'), may hold values from -0.125 to 0.125
- mix_branch: bfloat16 [2048, 1024], P('fs', 'tp'), may hold values from -0.125 to 0.125
- conv_weight: bfloat16 [4, 1024], P(None, 'tp'), may hold values from -3 to 3
- rate_weight: bfloat16 [16, 64, 64], P('tp'), may hold values from -0.75 to 0.75
- input_weight: bfloat16 [16, 64, 64], P('tp'), may hold values from -0.75 to 0.75
- decay_param: float32 [1024], P('tp'), may hold values from 3 to 11
- decay_shift: float32 [8192, 16], P('fs', 'tp'), may hold values from -1.5 to 0
- mix_output: bfloat16 [2048, 1024], P('fs', 'tp'), may hold values from -0.1875 to 0.1875
- second_gain: float32 [2048], replicated, may hold values from 0.1 to 1.9
- second_gate: bfloat16 [2048, 5120], P('fs', 'tp'), may hold values from -0.125 to 0.125
- second_up: bfloat16 [2048, 5120], P('fs', 'tp'), may hold values from -0.125 to 0.125
- second_down: bfloat16 [2048, 5120], P('fs', 'tp'), may hold values from -0.078125 to 0.078125
- final_gain: float32 [2048], P('tp'), may hold values from 0.1 to 1.9
Outputs:
- output: bfloat16 [8192, 2048], P('fs', 'tp')
The draws below stay inside these ranges and needn't reach their ends.
All inputs are finite; a program needn't handle non-finite values.
Results may differ from the reference program's by a relative error of at most 0.019.
Values may be sent and summed in bfloat16 or wider, within the bound.
A program may use at most 128 MiB of HBM per device.

```python
import math
import jax
import jax.numpy as jnp
from jax import lax

D = 2048
FF = 5120
LANE_GROUPINGS = 16
HEAD_DIM = 64
CONV = 4
SEQ = 1024
LRU = 1024
SYMBOL_TOTAL = 8192
N_TP = 4


def draw_tokens(key, part):
    key_base, key_rows = jax.random.split(key, 2)
    starting_number = jnp.clip(jax.random.normal(key_base, (SYMBOL_TOTAL, D), jnp.float32), -4.0, 4.0)
    rows = jnp.exp(jax.random.uniform(key_rows, (SYMBOL_TOTAL, 1), jnp.float32, 0.0, math.log(4.0)))
    columns = jnp.exp(math.log(3.0) * jnp.arange(D, dtype=jnp.float32) / D)
    return (0.25 * starting_number * rows * columns[None, :]).astype(jnp.bfloat16)


def draw_decay_param(key, part):
    key_pick, key_rate = jax.random.split(key, 2)
    share = 0.5
    picked = jax.random.uniform(key_pick, (LRU,), jnp.float32) < share
    unit = jax.random.uniform(key_rate, (LRU,), jnp.float32)
    slow = jnp.exp(math.log(0.5) + unit * math.log(4.0)) / (4.0 * SEQ)
    fast = jnp.exp(math.log(1.0 / 120.0) + unit * math.log(5.0))
    speed = jnp.where(picked, slow, fast)
    return -speed - jnp.log(-jnp.expm1(-speed))


def draw_decay_shift(key, part):
    key_base, key_spot, key_depth = jax.random.split(key, 3)
    count = SYMBOL_TOTAL // SEQ
    starting_number = -jnp.exp(jax.random.uniform(key_base, (count, 1, LANE_GROUPINGS), jnp.float32, math.log(0.1), math.log(0.5))) / SEQ
    location_marks = jax.random.randint(key_spot, (count, 2, 1), 0, SEQ)
    layer_ordinal = jnp.log(jax.random.uniform(key_depth, (count, 2, 1), jnp.float32, 0.5, 0.8))
    position_holders = jnp.arange(SEQ, dtype=jnp.int32)[None, None, :]
    repeated_spans = jnp.sum(jnp.where(location_marks == position_holders, layer_ordinal, 0.0), axis=1)
    return (starting_number + repeated_spans[:, :, None]).reshape(SYMBOL_TOTAL, LANE_GROUPINGS)


def steps_of(own_key, extent, pieces, low, largest):
    loudness, own = 1.0, jax.random.fold_in(own_key, 6)
    for axis_at, parts in pieces:
        steps = jnp.exp(jax.random.uniform(jax.random.fold_in(own, axis_at), (parts,), jnp.float32, low / len(pieces), largest / len(pieces)))
        loudness = loudness * jnp.repeat(steps, extent[axis_at] // parts).reshape([-1 if axis == axis_at else 1 for axis in range(len(extent))])
    return loudness


def noise(own_key, shape, spread, bound, cuts=(), kind=jnp.bfloat16):
    entries = jax.random.normal(own_key, shape, jnp.float32) * spread
    if len(cuts) > 0:
        entries = steps_of(own_key, shape, cuts, -0.22, 0.18) * entries
    return jnp.clip(entries, min=-bound, max=bound).astype(kind)


def setup_inputs(seed: int = 0) -> dict:
    streams_of = jax.random.split(jax.random.key(seed), 20)
    tokens = draw_tokens(jax.random.fold_in(streams_of[19], 71), 0)
    first_gain = jnp.clip(1.0 + 0.18 * jax.random.normal(streams_of[1], (D,), jnp.float32), 0.1, 1.9)
    first_gate = noise(streams_of[2], (D, FF), D ** -0.5, 0.125, ((0, 8), (1, 4)))
    first_up = noise(streams_of[3], (D, FF), D ** -0.5, 0.125, ((0, 8), (1, 4)))
    first_down = noise(streams_of[4], (D, FF), FF ** -0.5, 0.078125, ((0, 8), (1, 4)))
    mix_gain = jnp.clip(1.0 + 0.18 * jax.random.normal(streams_of[5], (D,), jnp.float32), 0.1, 1.9)
    mix_input = noise(streams_of[6], (D, LRU), D ** -0.5, 0.125, ((0, 8), (1, 4)))
    mix_branch = noise(streams_of[7], (D, LRU), D ** -0.5, 0.125, ((0, 8), (1, 4)))
    conv_weight = noise(streams_of[8], (CONV, LRU), CONV ** -0.5, 3.0, ((1, 4),))
    rate_weight = noise(streams_of[9], (LANE_GROUPINGS, HEAD_DIM, HEAD_DIM), HEAD_DIM ** -0.5, 0.75, ((0, 4),))
    input_weight = noise(streams_of[10], (LANE_GROUPINGS, HEAD_DIM, HEAD_DIM), HEAD_DIM ** -0.5, 0.75, ((0, 4),))
    decay_param = draw_decay_param(jax.random.fold_in(streams_of[19], 71), 0)
    decay_shift = draw_decay_shift(jax.random.fold_in(streams_of[19], 71), 0)
    mix_output = noise(streams_of[13], (D, LRU), LRU ** -0.5, 0.1875, ((0, 8), (1, 4)))
    second_gain = jnp.clip(1.0 + 0.18 * jax.random.normal(streams_of[14], (D,), jnp.float32), 0.1, 1.9)
    second_gate = noise(streams_of[15], (D, FF), D ** -0.5, 0.125, ((0, 8), (1, 4)))
    second_up = noise(streams_of[16], (D, FF), D ** -0.5, 0.125, ((0, 8), (1, 4)))
    second_down = noise(streams_of[17], (D, FF), FF ** -0.5, 0.078125, ((0, 8), (1, 4)))
    final_gain = jnp.clip(1.0 + 0.18 * jax.random.normal(streams_of[18], (D,), jnp.float32), 0.1, 1.9)
    return dict(tokens=tokens, first_gain=first_gain, first_gate=first_gate, first_up=first_up, first_down=first_down, mix_gain=mix_gain, mix_input=mix_input, mix_branch=mix_branch, conv_weight=conv_weight, rate_weight=rate_weight, input_weight=input_weight, decay_param=decay_param, decay_shift=decay_shift, mix_output=mix_output, second_gain=second_gain, second_gate=second_gate, second_up=second_up, second_down=second_down, final_gain=final_gain)


norm_eps = 1e-06
rate_scale = 8.0

def rms_rows(rows, gain):
    values = rows.astype(jnp.float32)
    scale = lax.rsqrt(lax.optimization_barrier(jnp.mean(values * values, axis=-1, keepdims=True)) + norm_eps)
    return (values * scale * gain).astype(jnp.bfloat16)

def group_terms(left, weight):
    width = left.shape[1] // N_TP
    total = jnp.zeros((left.shape[0], weight.shape[0]), jnp.float32)
    for group in range(N_TP):
        piece = left[:, group * width:(group + 1) * width]
        weight_piece = weight[:, group * width:(group + 1) * width]
        term = lax.dot_general(piece, weight_piece, (((1,), (1,)), ((), ())), preferred_element_type=jnp.float32)
        total = total + lax.optimization_barrier(term.astype(jnp.bfloat16)).astype(jnp.float32)
    return total

def half_step(stream, gain, weight_gate, weight_up, weight_down):
    normed = rms_rows(stream, gain)
    gate_value = jnp.dot(normed, weight_gate, preferred_element_type=jnp.float32)
    up_value = jnp.dot(normed, weight_up, preferred_element_type=jnp.float32)
    hidden = (jax.nn.silu(gate_value) * up_value).astype(jnp.bfloat16)
    return (stream.astype(jnp.float32) + 0.5 * group_terms(hidden, weight_down)).astype(jnp.bfloat16)

def combine_steps(earlier, later):
    return (earlier[0] * later[0], later[0] * earlier[1] + later[1])

def lane_mixer(stream, gain, mix_input, mix_branch, conv_weight, rate_weight, input_weight, decay_param, decay_shift, mix_output):
    normed = rms_rows(stream, gain)
    lane_input = jnp.dot(normed, mix_input, preferred_element_type=jnp.float32).astype(jnp.bfloat16)
    branch_value = jnp.dot(normed, mix_branch, preferred_element_type=jnp.float32)
    width = lane_input.shape[1]
    lanes = lane_input.reshape(-1, SEQ, width).astype(jnp.float32)
    count = lanes.shape[0]
    padded = jnp.pad(lanes, ((0, 0), (CONV - 1, 0), (0, 0)))
    conv_sum = jnp.zeros_like(lanes)
    for offset in range(CONV):
        conv_sum = conv_sum + padded[:, offset:offset + SEQ] * conv_weight[offset].astype(jnp.float32)
    conv_out = conv_sum.astype(jnp.bfloat16)
    blocks = conv_out.reshape(count, SEQ, -1, HEAD_DIM).astype(jnp.float32)
    rate = jax.nn.sigmoid(jnp.einsum('nshd,hde->nshe', blocks, rate_weight.astype(jnp.float32))).reshape(lanes.shape)
    admit = jax.nn.sigmoid(jnp.einsum('nshd,hde->nshe', blocks, input_weight.astype(jnp.float32))).reshape(lanes.shape)
    shift = jnp.repeat(decay_shift.reshape(count, SEQ, -1), HEAD_DIM, axis=-1)
    log_decay = rate_scale * rate * jax.nn.log_sigmoid(decay_param) + shift
    drive = jnp.sqrt(-jnp.expm1(2.0 * log_decay)) * admit * conv_out.astype(jnp.float32)
    _, state = lax.associative_scan(combine_steps, (jnp.exp(log_decay), drive), axis=1)
    mixed_lane = (state.reshape(-1, width) * jax.nn.gelu(branch_value)).astype(jnp.bfloat16)
    return (stream.astype(jnp.float32) + group_terms(mixed_lane, mix_output)).astype(jnp.bfloat16)

def reference(tokens, first_gain, first_gate, first_up, first_down, mix_gain, mix_input, mix_branch, conv_weight, rate_weight, input_weight, decay_param, decay_shift, mix_output, second_gain, second_gate, second_up, second_down, final_gain):
    stream = half_step(tokens, first_gain, first_gate, first_up, first_down)
    stream = lane_mixer(stream, mix_gain, mix_input, mix_branch, conv_weight, rate_weight, input_weight, decay_param, decay_shift, mix_output)
    stream = half_step(stream, second_gain, second_gate, second_up, second_down)
    values = stream.astype(jnp.float32)
    scale = lax.rsqrt(lax.optimization_barrier(jnp.mean(values * values, axis=-1, keepdims=True)) + norm_eps)
    return (values * scale * final_gain).astype(jnp.bfloat16)
```

```python
import jax
import jax.numpy as jnp
from jax import lax
from jax.experimental import pallas as pl
from jax.experimental.pallas import tpu as pltpu
from jax.sharding import PartitionSpec as P


D = 2048
HEAD_DIM = 64
CONV = 4
SEQ = 1024


norm_eps = 1e-06
rate_scale = 8.0


def rms_rows(rows, gain):
    values = rows.astype(jnp.float32)
    scale = lax.rsqrt(jnp.mean(values * values, axis=-1, keepdims=True) + norm_eps)
    return (values * scale * gain).astype(jnp.bfloat16)


def after(value, *earlier):
    return lax.optimization_barrier((value, *earlier))[0]


def put(whole, block, row):
    return lax.dynamic_update_slice(whole, block, (row, jnp.int32(0)))


def ring_gather(block):
    n = lax.axis_size("fs")
    rows, columns = block.shape
    order = list(range(0, n, 2)) + list(range(1, n, 2))[::-1]
    forward = [(order[i], order[(i + 1) % n]) for i in range(n)]
    backward = [(to, source) for source, to in forward]
    place = [order.index(i) for i in range(n)]
    me = lax.axis_index("fs")
    at = jnp.array(place, jnp.int32)[me]
    owners = jnp.array(order, jnp.int32)
    whole = put(jnp.zeros((n * rows, columns), block.dtype), block, me * rows)
    ahead, back = block, block
    for step in range(1, (n + 1) // 2):
        ahead = lax.ppermute(ahead, "fs", forward)
        back = lax.ppermute(back, "fs", backward)
        whole = put(whole, ahead, owners[(at - step) % n] * rows)
        whole = put(whole, back, owners[(at + step) % n] * rows)
    if n % 2 == 0:
        half = rows // 2
        base = owners[(at + n // 2) % n] * rows
        ahead = lax.ppermute(ahead[:half], "fs", forward)
        back = lax.ppermute(back[half:], "fs", backward)
        whole = put(whole, ahead, base)
        whole = put(whole, back, base + half)
    return whole, (ahead, back)


def tp_maps():
    n = lax.axis_size("tp")
    chips = n // 2
    partner = [(i, i ^ 1) for i in range(n)]
    hops = [[(i, (i + 2 * d) % n) for i in range(n)] for d in range(1, chips)]
    return n, chips, partner, hops


def full_rows(stream, gain):
    n, chips, partner, hops = tp_maps()
    me = lax.axis_index("tp")
    width = stream.shape[1]
    far = [lax.ppermute(stream, "tp", hop) for hop in hops]
    whole = jnp.zeros((stream.shape[0], n * width), stream.dtype)
    blocks = [(stream, 0)] + [(far[d - 1], 2 * d) for d in range(1, chips)]
    for block, back in blocks:
        owner = (me - back) % n
        near = lax.ppermute(block, "tp", partner)
        whole = lax.dynamic_update_slice(whole, block, (jnp.int32(0), owner * width))
        whole = lax.dynamic_update_slice(whole, near, (jnp.int32(0), (owner ^ 1) * width))
    return rms_rows(whole, gain)


def reduce_back(partial_value):
    n, chips, partner, hops = tp_maps()
    me = lax.axis_index("tp")
    width = partial_value.shape[1] // n

    def block(owner):
        return lax.dynamic_slice_in_dim(partial_value, owner * width, width, axis=1)

    sums = []
    for d in list(range(1, chips)) + [0]:
        owner = (me + 2 * d) % n
        sent = block(owner ^ 1)
        near = lax.ppermute(sent, "tp", partner)
        sums.append(block(owner).astype(jnp.float32) + near.astype(jnp.float32))
    total = sums[-1]
    for d in range(1, chips):
        sent = sums[d - 1].astype(jnp.bfloat16)
        arrived = lax.ppermute(sent, "tp", hops[d - 1])
        total = total + arrived.astype(jnp.float32)
    return total


def contract_last(left, right):
    return lax.dot_general(
        left, right, (((1,), (1,)), ((), ())), preferred_element_type=jnp.float32
    )


def half_step(stream, gain, whole_gate, whole_up, whole_down):
    normed = full_rows(stream, gain)
    gate_value = jnp.dot(normed, whole_gate, preferred_element_type=jnp.float32)
    up_value = jnp.dot(normed, whole_up, preferred_element_type=jnp.float32)
    hidden = (jax.nn.silu(gate_value) * up_value).astype(jnp.bfloat16)
    partial_value = contract_last(hidden, whole_down).astype(jnp.bfloat16)
    total = reduce_back(partial_value)
    return (stream.astype(jnp.float32) + 0.5 * total).astype(jnp.bfloat16)


def scan_kernel(decay_ref, drive_ref, state_ref):
    decay, drive = decay_ref[...], drive_ref[...]
    rows = decay.shape[0]
    row = lax.broadcasted_iota(jnp.int32, decay.shape, 0)
    shift = 1
    while shift < rows:
        inside = row >= shift
        before_decay = jnp.where(inside, pltpu.roll(decay, shift, 0), 1.0)
        before_drive = jnp.where(inside, pltpu.roll(drive, shift, 0), 0.0)
        drive = decay * before_drive + drive
        decay = decay * before_decay
        shift *= 2
    state_ref[...] = drive


def scan_states(decay, drive):
    rows, width = decay.shape
    lanes = min(width, 128)
    spec = pl.BlockSpec((SEQ, lanes), lambda i, j: (i, j))
    return pl.pallas_call(
        scan_kernel,
        grid=(rows // SEQ, width // lanes),
        in_specs=[spec, spec],
        out_specs=spec,
        out_shape=jax.ShapeDtypeStruct((rows, width), jnp.float32),
        cost_estimate=pl.CostEstimate(
            flops=rows * width * 60, bytes_accessed=rows * width * 12, transcendentals=0
        ),
    )(decay, drive)


def lane_mixer(
    stream,
    gain,
    whole_input,
    whole_branch,
    conv_weight,
    rate_weight,
    input_weight,
    decay_param,
    decay_shift,
    whole_output,
):
    normed = full_rows(stream, gain)
    lane_input = jnp.dot(normed, whole_input, preferred_element_type=jnp.float32).astype(
        jnp.bfloat16
    )
    branch_value = jnp.dot(normed, whole_branch, preferred_element_type=jnp.float32)
    width = lane_input.shape[1]
    lanes = lane_input.reshape(-1, SEQ, width).astype(jnp.float32)
    count = lanes.shape[0]
    padded = jnp.pad(lanes, ((0, 0), (CONV - 1, 0), (0, 0)))
    conv_sum = jnp.zeros_like(lanes)
    for offset in range(CONV):
        conv_sum = conv_sum + padded[:, offset : offset + SEQ] * conv_weight[offset].astype(
            jnp.float32
        )
    conv_out = conv_sum.astype(jnp.bfloat16)
    blocks = conv_out.reshape(count, SEQ, -1, HEAD_DIM)
    rate = jax.nn.sigmoid(
        jnp.einsum("nshd,hde->nshe", blocks, rate_weight, preferred_element_type=jnp.float32)
    ).reshape(lanes.shape)
    admit = jax.nn.sigmoid(
        jnp.einsum("nshd,hde->nshe", blocks, input_weight, preferred_element_type=jnp.float32)
    ).reshape(lanes.shape)
    shift = jnp.repeat(decay_shift.reshape(count, SEQ, -1), HEAD_DIM, axis=-1)
    log_decay = rate_scale * rate * jax.nn.log_sigmoid(decay_param) + shift
    drive = jnp.sqrt(-jnp.expm1(2.0 * log_decay)) * admit * conv_out.astype(jnp.float32)
    state = scan_states(jnp.exp(log_decay).reshape(-1, width), drive.reshape(-1, width))
    mixed_lane = (state * jax.nn.gelu(branch_value)).astype(jnp.bfloat16)
    partial_value = contract_last(mixed_lane, whole_output).astype(jnp.bfloat16)
    total = reduce_back(partial_value)
    return (stream.astype(jnp.float32) + total).astype(jnp.bfloat16)


def shards(
    tokens,
    first_gain,
    first_gate,
    first_up,
    first_down,
    mix_gain,
    mix_input,
    mix_branch,
    conv_weight,
    rate_weight,
    input_weight,
    decay_param,
    decay_shift,
    mix_output,
    second_gain,
    second_gate,
    second_up,
    second_down,
    final_gain,
):
    lanes = mix_input.shape[1]
    units = first_down.shape[1]
    first, done = ring_gather(jnp.concatenate([first_gate, first_up], axis=1))
    down, done = ring_gather(after(first_down, *done))
    rest = jnp.concatenate([mix_input, mix_branch, mix_output, second_gate], axis=1)
    rest, done = ring_gather(after(rest, *done))
    last = jnp.concatenate([second_up, second_down], axis=1)
    last, done = ring_gather(after(last, *done))
    stream = half_step(tokens, first_gain, first[:, :units], first[:, units:], down)
    stream = lane_mixer(
        stream,
        mix_gain,
        rest[:, :lanes],
        rest[:, lanes : 2 * lanes],
        conv_weight,
        rate_weight,
        input_weight,
        decay_param,
        decay_shift,
        rest[:, 2 * lanes : 3 * lanes],
    )
    stream = half_step(stream, second_gain, rest[:, 3 * lanes :], last[:, :units], last[:, units:])
    values = stream.astype(jnp.float32)
    squares = lax.psum(jnp.sum(values * values, axis=1), "tp")
    scale = lax.rsqrt(squares / D + norm_eps)
    return (values * scale[:, None] * final_gain).astype(jnp.bfloat16)


def solution(mesh):
    return jax.shard_map(
        shards,
        mesh=mesh,
        in_specs=(
            P("fs", "tp"),
            P(),
            P("fs", "tp"),
            P("fs", "tp"),
            P("fs", "tp"),
            P(),
            P("fs", "tp"),
            P("fs", "tp"),
            P(None, "tp"),
            P("tp", None, None),
            P("tp", None, None),
            P("tp"),
            P("fs", "tp"),
            P("fs", "tp"),
            P(),
            P("fs", "tp"),
            P("fs", "tp"),
            P("fs", "tp"),
            P("tp"),
        ),
        out_specs=P("fs", "tp"),
        check_vma=False,
    )
```

```python
import jax
import jax.numpy as jnp
from jax import lax
from jax.experimental import pallas as pl
from jax.experimental.pallas import tpu as pltpu
from jax.sharding import PartitionSpec as P


D = 2048
HEAD_DIM = 64
CONV = 4
SEQ = 1024


norm_eps = 1e-06
rate_scale = 8.0


def rms_rows(rows, gain):
    values = rows.astype(jnp.float32)
    scale = lax.rsqrt(jnp.mean(values * values, axis=-1, keepdims=True) + norm_eps)
    return (values * scale * gain).astype(jnp.bfloat16)


def after(value, *earlier):
    return lax.optimization_barrier((value, *earlier))[0]


def put(whole, block, row):
    return lax.dynamic_update_slice(whole, block, (row, jnp.int32(0)))


def ring_gather(block):
    n = lax.axis_size("fs")
    rows, columns = block.shape
    order = list(range(0, n, 2)) + list(range(1, n, 2))[::-1]
    forward = [(order[i], order[(i + 1) % n]) for i in range(n)]
    backward = [(to, source) for source, to in forward]
    place = [order.index(i) for i in range(n)]
    me = lax.axis_index("fs")
    at = jnp.array(place, jnp.int32)[me]
    owners = jnp.array(order, jnp.int32)
    whole = put(jnp.zeros((n * rows, columns), block.dtype), block, me * rows)
    ahead, back = block, block
    for step in range(1, (n + 1) // 2):
        ahead = lax.ppermute(ahead, "fs", forward)
        back = lax.ppermute(back, "fs", backward)
        whole = put(whole, ahead, owners[(at - step) % n] * rows)
        whole = put(whole, back, owners[(at + step) % n] * rows)
    if n % 2 == 0:
        half = rows // 2
        base = owners[(at + n // 2) % n] * rows
        ahead = lax.ppermute(ahead[:half], "fs", forward)
        back = lax.ppermute(back[half:], "fs", backward)
        whole = put(whole, ahead, base)
        whole = put(whole, back, base + half)
    return whole, (ahead, back)


def tp_maps():
    n = lax.axis_size("tp")
    chips = n // 2
    partner = [(i, i ^ 1) for i in range(n)]
    hops = [[(i, (i + 2 * d) % n) for i in range(n)] for d in range(1, chips)]
    return n, chips, partner, hops


def ring_down(hidden, block):
    n = lax.axis_size("fs")
    rows = block.shape[0]
    order = list(range(0, n, 2)) + list(range(1, n, 2))[::-1]
    forward = [(order[i], order[(i + 1) % n]) for i in range(n)]
    backward = [(to, source) for source, to in forward]
    place = [order.index(i) for i in range(n)]
    me = lax.axis_index("fs")
    at = jnp.array(place, jnp.int32)[me]
    owners = jnp.array(order, jnp.int32)
    pieces = jnp.zeros((n, hidden.shape[0], rows), jnp.bfloat16)

    def place_terms(pieces, weight, owner):
        terms = contract_last(hidden, weight).astype(jnp.bfloat16)
        return lax.dynamic_update_slice(pieces, terms[None], (owner, jnp.int32(0), jnp.int32(0)))

    pieces = place_terms(pieces, block, me)
    ahead, back = block, block
    for step in range(1, (n + 1) // 2):
        ahead = lax.ppermute(ahead, "fs", forward)
        back = lax.ppermute(back, "fs", backward)
        pieces = place_terms(pieces, ahead, owners[(at - step) % n])
        pieces = place_terms(pieces, back, owners[(at + step) % n])
    if n % 2 == 0:
        half = rows // 2
        ahead = lax.ppermute(ahead[:half], "fs", forward)
        back = lax.ppermute(back[half:], "fs", backward)
        whole = jnp.concatenate([ahead, back], axis=0)
        pieces = place_terms(pieces, whole, owners[(at + n // 2) % n])
    return pieces, (ahead, back)


def full_rows(stream, gain):
    n, chips, partner, hops = tp_maps()
    me = lax.axis_index("tp")
    width = stream.shape[1]
    far = [lax.ppermute(stream, "tp", hop) for hop in hops]
    whole = jnp.zeros((stream.shape[0], n * width), stream.dtype)
    blocks = [(stream, 0)] + [(far[d - 1], 2 * d) for d in range(1, chips)]
    for block, back in blocks:
        owner = (me - back) % n
        near = lax.ppermute(block, "tp", partner)
        whole = lax.dynamic_update_slice(whole, block, (jnp.int32(0), owner * width))
        whole = lax.dynamic_update_slice(whole, near, (jnp.int32(0), (owner ^ 1) * width))
    return rms_rows(whole, gain)


def reduce_back(pieces, axis):
    n, chips, partner, hops = tp_maps()
    me = lax.axis_index("tp")
    width = pieces.shape[axis] // n

    def block(owner):
        return lax.dynamic_slice_in_dim(pieces, owner * width, width, axis=axis)

    sums = []
    for d in list(range(1, chips)) + [0]:
        owner = (me + 2 * d) % n
        sent = block(owner ^ 1)
        near = lax.ppermute(sent, "tp", partner)
        sums.append(block(owner).astype(jnp.float32) + near.astype(jnp.float32))
    total = sums[-1]
    for d in range(1, chips):
        sent = sums[d - 1].astype(jnp.bfloat16)
        arrived = lax.ppermute(sent, "tp", hops[d - 1])
        total = total + arrived.astype(jnp.float32)
    return total


def contract_last(left, right):
    return lax.dot_general(
        left, right, (((1,), (1,)), ((), ())), preferred_element_type=jnp.float32
    )


def hidden_of(stream, gain, whole_gate, whole_up):
    normed = full_rows(stream, gain)
    gate_value = jnp.dot(normed, whole_gate, preferred_element_type=jnp.float32)
    up_value = jnp.dot(normed, whole_up, preferred_element_type=jnp.float32)
    return (jax.nn.silu(gate_value) * up_value).astype(jnp.bfloat16)


def add_half(stream, total):
    return (stream.astype(jnp.float32) + 0.5 * total).astype(jnp.bfloat16)


def scan_kernel(decay_ref, drive_ref, state_ref):
    decay, drive = decay_ref[...], drive_ref[...]
    rows = decay.shape[0]
    row = lax.broadcasted_iota(jnp.int32, decay.shape, 0)
    shift = 1
    while shift < rows:
        inside = row >= shift
        before_decay = jnp.where(inside, pltpu.roll(decay, shift, 0), 1.0)
        before_drive = jnp.where(inside, pltpu.roll(drive, shift, 0), 0.0)
        drive = decay * before_drive + drive
        decay = decay * before_decay
        shift *= 2
    state_ref[...] = drive


def scan_states(decay, drive):
    rows, width = decay.shape
    lanes = min(width, 128)
    spec = pl.BlockSpec((SEQ, lanes), lambda i, j: (i, j))
    return pl.pallas_call(
        scan_kernel,
        grid=(rows // SEQ, width // lanes),
        in_specs=[spec, spec],
        out_specs=spec,
        out_shape=jax.ShapeDtypeStruct((rows, width), jnp.float32),
        cost_estimate=pl.CostEstimate(
            flops=rows * width * 60, bytes_accessed=rows * width * 12, transcendentals=0
        ),
    )(decay, drive)


def lane_mixer(
    stream,
    gain,
    whole_input,
    whole_branch,
    conv_weight,
    rate_weight,
    input_weight,
    decay_param,
    decay_shift,
    whole_output,
):
    normed = full_rows(stream, gain)
    lane_input = jnp.dot(normed, whole_input, preferred_element_type=jnp.float32).astype(
        jnp.bfloat16
    )
    branch_value = jnp.dot(normed, whole_branch, preferred_element_type=jnp.float32)
    width = lane_input.shape[1]
    lanes = lane_input.reshape(-1, SEQ, width).astype(jnp.float32)
    count = lanes.shape[0]
    padded = jnp.pad(lanes, ((0, 0), (CONV - 1, 0), (0, 0)))
    conv_sum = jnp.zeros_like(lanes)
    for offset in range(CONV):
        conv_sum = conv_sum + padded[:, offset : offset + SEQ] * conv_weight[offset].astype(
            jnp.float32
        )
    conv_out = conv_sum.astype(jnp.bfloat16)
    blocks = conv_out.reshape(count, SEQ, -1, HEAD_DIM)
    rate = jax.nn.sigmoid(
        jnp.einsum("nshd,hde->nshe", blocks, rate_weight, preferred_element_type=jnp.float32)
    ).reshape(lanes.shape)
    admit = jax.nn.sigmoid(
        jnp.einsum("nshd,hde->nshe", blocks, input_weight, preferred_element_type=jnp.float32)
    ).reshape(lanes.shape)
    shift = jnp.repeat(decay_shift.reshape(count, SEQ, -1), HEAD_DIM, axis=-1)
    log_decay = rate_scale * rate * jax.nn.log_sigmoid(decay_param) + shift
    drive = jnp.sqrt(-jnp.expm1(2.0 * log_decay)) * admit * conv_out.astype(jnp.float32)
    state = scan_states(jnp.exp(log_decay).reshape(-1, width), drive.reshape(-1, width))
    mixed_lane = (state * jax.nn.gelu(branch_value)).astype(jnp.bfloat16)
    partial_value = contract_last(mixed_lane, whole_output).astype(jnp.bfloat16)
    total = reduce_back(partial_value, 1)
    return (stream.astype(jnp.float32) + total).astype(jnp.bfloat16)


def shards(
    tokens,
    first_gain,
    first_gate,
    first_up,
    first_down,
    mix_gain,
    mix_input,
    mix_branch,
    conv_weight,
    rate_weight,
    input_weight,
    decay_param,
    decay_shift,
    mix_output,
    second_gain,
    second_gate,
    second_up,
    second_down,
    final_gain,
):
    lanes = mix_input.shape[1]
    units = first_down.shape[1]
    first, done = ring_gather(jnp.concatenate([first_gate, first_up], axis=1))
    hidden = hidden_of(tokens, first_gain, first[:, :units], first[:, units:])
    pieces, done = ring_down(hidden, after(first_down, *done))
    rest = jnp.concatenate([mix_input, mix_branch, mix_output], axis=1)
    rest, done = ring_gather(after(rest, *done))
    second = jnp.concatenate([second_gate, second_up], axis=1)
    second, done = ring_gather(after(second, *done))
    down, done = ring_gather(after(second_down, *done))
    total = reduce_back(pieces, 0)
    stream = add_half(tokens, total.transpose(1, 0, 2).reshape(tokens.shape))
    stream = lane_mixer(
        stream,
        mix_gain,
        rest[:, :lanes],
        rest[:, lanes : 2 * lanes],
        conv_weight,
        rate_weight,
        input_weight,
        decay_param,
        decay_shift,
        rest[:, 2 * lanes : 3 * lanes],
    )
    hidden = hidden_of(stream, second_gain, second[:, :units], second[:, units:])
    rows = hidden.shape[0] // 2
    totals = []
    for part in range(2):
        terms = contract_last(hidden[part * rows : (part + 1) * rows], down)
        terms = terms.astype(jnp.bfloat16)
        totals.append(reduce_back(terms, 1))
    stream = add_half(stream, jnp.concatenate(totals, axis=0))
    values = stream.astype(jnp.float32)
    squares = lax.psum(jnp.sum(values * values, axis=1), "tp")
    scale = lax.rsqrt(squares / D + norm_eps)
    return (values * scale[:, None] * final_gain).astype(jnp.bfloat16)


def solution(mesh):
    return jax.shard_map(
        shards,
        mesh=mesh,
        in_specs=(
            P("fs", "tp"),
            P(),
            P("fs", "tp"),
            P("fs", "tp"),
            P("fs", "tp"),
            P(),
            P("fs", "tp"),
            P("fs", "tp"),
            P(None, "tp"),
            P("tp", None, None),
            P("tp", None, None),
            P("tp"),
            P("fs", "tp"),
            P("fs", "tp"),
            P(),
            P("fs", "tp"),
            P("fs", "tp"),
            P("fs", "tp"),
            P("tp"),
        ),
        out_specs=P("fs", "tp"),
        check_vma=False,
    )
```
